32 devices in a mesh: grp: 2 (over x), ep: 16 (over z, y, core).
Axes of the slice: x: 2, y: 2, z: 4, core: 2. Of those that a mesh axis runs over, the one named last changes fastest.
Arguments:
- tokens: bfloat16 [4096, 2048], P(('grp', 'ep')), parts along dimension 0, may hold values from -6 to 6
- routing: int32 [4096, 2], P(('grp', 'ep')), parts along dimension 0, may hold values from 0 to 3, all different within a row; in each aligned block of 128 rows (0 to 127, 128 to 255, ...) at most 80 rows name the same one
- gates: float32 [4096, 2], P(('grp', 'ep')), parts along dimension 0, may hold values from 0.2 to 1
- norm_gain: bfloat16 [2048], replicated, may hold values from 0.099609375 to 1.8984375
- w_gate: bfloat16 [16, 2048, 896], P('ep'), may hold values from -0.125 to 0.125
- w_up: bfloat16 [16, 2048, 896], P('ep'), may hold values from -0.125 to 0.125
- w_down: bfloat16 [16, 896, 2048], P('ep'), may hold values from -0.09375 to 0.09375
Outputs:
- mixed: bfloat16 [4096, 2048], P(('grp', 'ep')), parts along dimension 0
The draws below stay inside these ranges and needn't reach their ends.
There are 2 independent parts, one for each index of `grp`. The reference program is written for one: setup_inputs(seed, part) draws one part's arguments, and reference() takes and returns one part's arrays. A program takes and returns all parts, laid end to end along the dimension named above; an argument that names none is the same for every part. Nothing has to cross between parts.
Inputs may be any that keep to these rules, and one draw needn't show every extreme that they name: `routing`: each row names 2 different experts. Among the rows of one device at most 80 name any one expert, and in every draw some expert is named by exactly 80 rows of some device.
All inputs are finite; a program needn't handle non-finite values.
Results may differ from the reference program's by a relative error of at most 0.0078.
Values may be sent and summed in bfloat16 or wider, within the bound.
No kernel may reach another device: no remote copies, remote signals or barrier semaphores. Data moves between devices by JAX's collectives and lax.ppermute only.
A program may use at most 128 MiB of HBM per device.

```python
import math
import jax
import jax.numpy as jnp
import numpy as np
from jax import lax

D = 2048
FF = 3584
TOP = 2
GROUP = 4
TOK_DEV = 128
EXPERTS = 4
CAP = 80
TOKENS = 2048
N_EP = 16


def levels(key, dims, pieces, low, top_value):
    factor_of, own = 1.0, jax.random.fold_in(key, 6)
    for axis_at, blocks in pieces:
        steps = jnp.exp(jax.random.uniform(jax.random.fold_in(own, axis_at), (blocks,), jnp.float32, low / len(pieces), top_value / len(pieces)))
        factor_of = factor_of * jnp.repeat(steps, dims[axis_at] // blocks).reshape([-1 if axis == axis_at else 1 for axis in range(len(dims))])
    return factor_of


def assign_block(own_key, own, number, rows, number_of, top, bound, lean):
    order = jax.random.permutation(own_key, number_of)
    heavy_load, common = load_shares(number_of, rows * top, bound, lean, True), load_shares(number_of, rows * top, bound, lean, False)
    places = jnp.arange(number_of)

    def named(sizes, offset_by):
        used = int((sizes > 0).sum())
        fixed = max(1, used // 4)
        passed = fixed + (places - fixed + offset_by * (used - fixed)) % max(1, number_of - fixed)
        return jnp.zeros((number_of,), jnp.int32).at[order[jnp.where(places < fixed, places, passed)]].set(jnp.asarray(sizes, jnp.int32))

    sizes = jnp.where(number % 4 == 0, named(heavy_load, number // 4), named(common, number - number // 4 - 1))
    mixed = jax.random.permutation(jax.random.fold_in(own, 3), number_of)
    donor, taker = mixed[0:number_of // 2 * 2:2], mixed[1:number_of // 2 * 2:2]
    room = jnp.minimum(sizes[donor] - 1, bound - sizes[taker]) // 2
    room = jnp.where((donor == order[0]) | (taker == order[0]) | (sizes[taker] == 0), 0, jnp.maximum(room, 0))
    passed = jax.random.randint(jax.random.fold_in(own, 4), (number_of // 2,), 0, 1 << 20) % (room + 1)
    sizes = sizes.at[donor].add(-passed).at[taker].add(passed)
    labels = jnp.searchsorted(jnp.cumsum(sizes), jnp.arange(rows * top), side="right").astype(jnp.int32)
    table = labels.reshape(top, rows).T
    table = table[jax.random.permutation(jax.random.fold_in(own, 1), rows)]
    offset_by = jax.random.randint(jax.random.fold_in(own, 2), (rows, 1), 0, top)
    return jnp.take_along_axis(table, (jnp.arange(top)[None, :] + offset_by) % top, axis=1)


def load_shares(number_of, total, bound, skew, full):
    portions = [(1 << 20) // math.isqrt(grade ** skew) + 1 for grade in range(1, number_of + 1)]
    largest = bound if full else min(bound, max(-(-total // number_of), total * portions[0] // sum(portions)))
    least = 1 if total - largest >= number_of - 1 else 0
    given, spare = [largest] + [least] * (number_of - 1), total - largest - least * (number_of - 1)
    while spare > 0:
        free = [i for i in range(1, number_of) if given[i] < largest] or [i for i in range(1, number_of) if given[i] < bound]
        pool, left = sum([portions[i] for i in free]), spare
        for i in free:
            extra = min(bound - given[i], max(1, left * portions[i] // pool), spare)
            given[i] = given[i] + extra
            spare = spare - extra
    return np.array(given)


def normal_values(rng, shape, deviation, limit, pieces=(), kind=jnp.bfloat16):
    values = deviation * jax.random.normal(rng, shape, jnp.float32)
    if pieces:
        values = values * levels(rng, shape, pieces, -0.22, 0.18)
    return jnp.clip(values, -limit, limit).astype(kind)


def setup_inputs(seed: int = 0, part: int = 0) -> dict:
    key_of = jax.random.split(jax.random.key(seed), 8)
    own_keys = jax.random.split(jax.random.fold_in(key_of[7], part), 8)
    tokens = normal_values(own_keys[0], (TOKENS, D), 1.0, 6.0, ((0, 16),))
    routing_keys = jax.random.split(jax.random.fold_in(own_keys[1], 1), TOKENS // TOK_DEV)
    routing_turns = jax.random.permutation(jax.random.fold_in(own_keys[1], 3), TOKENS // TOK_DEV)
    routing = jax.vmap(lambda own, number: assign_block(jax.random.fold_in(own_keys[1], 2), own, number, TOK_DEV, EXPERTS, TOP, CAP, 2))(routing_keys, routing_turns).reshape((TOKENS, TOP))
    gates = jnp.clip(0.2 + 0.8 * jax.random.uniform(own_keys[2], (TOKENS, TOP), jnp.float32) ** levels(own_keys[2], (TOKENS, TOP), ((0, 16),), -0.2, 0.2), 0.2, 1.0)
    norm_gain = jnp.clip(1.0 + 0.18 * jax.random.normal(key_of[3], (D,), jnp.float32), 0.099609375, 1.8984375).astype(jnp.bfloat16)
    w_gate = normal_values(key_of[4], (N_EP, D, FF // GROUP), D ** -0.5, 0.125, ((0, 16),))
    w_up = normal_values(key_of[5], (N_EP, D, FF // GROUP), D ** -0.5, 0.125, ((0, 16),))
    w_down = normal_values(key_of[6], (N_EP, FF // GROUP, D), FF ** -0.5, 0.09375, ((0, 16),))
    return dict(tokens=tokens, routing=routing, gates=gates, norm_gain=norm_gain, w_gate=w_gate, w_up=w_up, w_down=w_down)


def run_expert(operands):
    expert_rows, gate_piece, up_piece, down_piece = operands
    gate_matrix = jnp.moveaxis(gate_piece, 0, 1).reshape(D, FF)
    up_matrix = jnp.moveaxis(up_piece, 0, 1).reshape(D, FF)
    gate_act = jnp.dot(expert_rows, gate_matrix, preferred_element_type=jnp.float32)
    up_act = jnp.dot(expert_rows, up_matrix, preferred_element_type=jnp.float32)
    hidden = (jax.nn.silu(gate_act) * up_act).astype(jnp.bfloat16)
    return jnp.dot(hidden, down_piece, preferred_element_type=jnp.float32).astype(jnp.bfloat16)

def reference(tokens, routing, gates, norm_gain, w_gate, w_up, w_down):
    values = tokens.astype(jnp.float32)
    scale = lax.rsqrt(lax.optimization_barrier(jnp.mean(values * values, axis=-1, keepdims=True)) + 1e-06)
    normed = (values * scale * norm_gain.astype(jnp.float32)).astype(jnp.bfloat16)
    blocks = routing.reshape(N_EP, TOK_DEV, TOP).astype(jnp.int32)
    one_hot = (blocks[..., None] == jnp.arange(EXPERTS, dtype=jnp.int32)).astype(jnp.int32)
    per_token = lax.optimization_barrier(jnp.sum(one_hot, axis=2)).astype(jnp.int32)
    before = (jnp.cumsum(per_token, axis=1) - per_token).astype(jnp.int32)
    slots = lax.optimization_barrier(jnp.sum(one_hot * before[:, :, None, :], axis=-1)).astype(jnp.int32)
    source = jnp.arange(N_EP, dtype=jnp.int32)[:, None, None]
    target = ((blocks * N_EP + source) * CAP + slots).reshape(-1).astype(jnp.int32)
    filled = jnp.zeros((EXPERTS * N_EP * CAP, D), jnp.bfloat16)
    filled = filled.at[target].set(jnp.repeat(normed, TOP, axis=0))
    expert_rows = filled.reshape(EXPERTS, N_EP * CAP, D)
    gate_pieces = w_gate.reshape(EXPERTS, GROUP, D, FF // GROUP)
    up_pieces = w_up.reshape(EXPERTS, GROUP, D, FF // GROUP)
    down_pieces = w_down.reshape(EXPERTS, FF, D)
    results = lax.map(run_expert, (expert_rows, gate_pieces, up_pieces, down_pieces))
    picked = results.reshape(EXPERTS * N_EP * CAP, D)[target].reshape(N_EP * TOK_DEV, TOP, D)
    mixed = lax.optimization_barrier(jnp.sum(gates[..., None] * picked.astype(jnp.float32), axis=1))
    return mixed.astype(jnp.bfloat16)
```

```python
import functools
import jax
import jax.numpy as jnp
from jax import lax
from jax.experimental import pallas as pl
from jax.experimental.pallas import tpu as pltpu
from jax.sharding import PartitionSpec as P

GROUP = 4
MAX_CHUNKS = 4
VMEM = pltpu.VMEM
SMEM = pltpu.SMEM


def expert_of(place, distance, experts):
    return lax.rem(place + distance, experts)


def prepare_body(experts, capacity, place_ref, tokens_ref, routing_ref, gain_ref, slot_ref, *block_refs):
    tok_count = tokens_ref.shape[0]
    top_count = routing_ref.shape[1]
    place = place_ref[0]
    values = tokens_ref[...].astype(jnp.float32)
    scale = lax.rsqrt(jnp.mean(values * values, axis=-1, keepdims=True) + 1e-06)
    normed = (values * scale * gain_ref[...].astype(jnp.float32)).astype(jnp.bfloat16)
    routing = routing_ref[...]
    expert_iota = lax.broadcasted_iota(jnp.int32, (tok_count, experts), 1)
    named = jnp.zeros((tok_count, experts), jnp.float32)
    for k in range(top_count):
        named = named + (routing[:, k : k + 1] == expert_iota).astype(jnp.float32)
    earlier = (
        lax.broadcasted_iota(jnp.int32, (tok_count, tok_count), 1)
        < lax.broadcasted_iota(jnp.int32, (tok_count, tok_count), 0)
    ).astype(jnp.bfloat16)
    before = jnp.dot(earlier, named.astype(jnp.bfloat16), preferred_element_type=jnp.float32)
    columns = [
        jnp.sum(jnp.where(routing[:, k : k + 1] == expert_iota, before, 0.0), axis=1, keepdims=True)
        for k in range(top_count)
    ]
    top_iota = lax.broadcasted_iota(jnp.int32, (tok_count, top_count), 1)
    slots = jnp.zeros((tok_count, top_count), jnp.float32)
    for k in range(top_count):
        slots = jnp.where(top_iota == k, columns[k], slots)
    slot_ref[...] = slots.astype(jnp.int32)
    slot_iota = lax.broadcasted_iota(jnp.int32, (tok_count, capacity), 1)
    per_chunk = experts // len(block_refs)
    for d in range(experts):
        expert = expert_of(place, d, experts)
        mine = expert_iota == expert
        position = jnp.sum(jnp.where(mine, before, 0.0), axis=1, keepdims=True)
        here = jnp.sum(jnp.where(mine, named, 0.0), axis=1, keepdims=True)
        position = jnp.where(here > 0.0, position, -1.0).astype(jnp.int32)
        chosen = (position == slot_iota).astype(jnp.bfloat16)
        rows = lax.dot_general(
            chosen, normed, (((0,), (0,)), ((), ())), preferred_element_type=jnp.float32
        ).astype(jnp.bfloat16)
        block_refs[d // per_chunk][d % per_chunk] = rows


def expert_body(
    own_ref, other_ref, g0, g1, u0, u1, d0, d1, keep_ref, send_ref, rows, hidden, gates, ups, downs, sems
):
    half = own_ref.shape[0] * own_ref.shape[1]
    width = own_ref.shape[2]
    units = g0.shape[-1]
    copies = []
    for p, (g, u) in enumerate(((g0, u0), (g1, u1))):
        copies.append(pltpu.make_async_copy(g.at[0], gates.at[p], sems.at[0, p]))
        copies.append(pltpu.make_async_copy(u.at[0], ups.at[p], sems.at[1, p]))
    for p, d in enumerate((d0, d1)):
        copies.append(pltpu.make_async_copy(d.at[0], downs.at[pl.ds(p * units, units)], sems.at[2, p]))
    for copy in copies:
        copy.start()
    rows[:half] = own_ref[...].reshape(half, width)
    rows[half:] = other_ref[...].reshape(half, width)
    for p in range(2):
        copies[2 * p].wait()
        gate_act = jnp.dot(rows[...], gates[p], preferred_element_type=jnp.float32)
        copies[2 * p + 1].wait()
        up_act = jnp.dot(rows[...], ups[p], preferred_element_type=jnp.float32)
        hidden[:, p * units : (p + 1) * units] = (
            gate_act / (1.0 + jnp.exp(-gate_act)) * up_act
        ).astype(jnp.bfloat16)
    copies[4].wait()
    copies[5].wait()
    result = jnp.dot(hidden[...], downs[...], preferred_element_type=jnp.float32).astype(jnp.bfloat16)
    keep_ref[...] = result[:half].reshape(keep_ref.shape)
    send_ref[...] = result[half:].reshape(send_ref.shape)


def mix_body(experts, place_ref, routing_ref, slot_ref, gates_ref, *refs):
    *block_refs, out_ref = refs
    tok_count, top_count = routing_ref.shape
    capacity = block_refs[0].shape[1]
    per_chunk = experts // len(block_refs)
    place = place_ref[0]
    routing, slots, gates = routing_ref[...], slot_ref[...], gates_ref[...]
    slot_iota = lax.broadcasted_iota(jnp.int32, (tok_count, capacity), 1)
    total = jnp.zeros(out_ref.shape, jnp.float32)
    for k in range(top_count):
        picked = jnp.zeros(out_ref.shape, jnp.float32)
        for d in range(experts):
            expert = expert_of(place, d, experts)
            at = jnp.where(routing[:, k : k + 1] == expert, slots[:, k : k + 1], -1)
            chosen = (at == slot_iota).astype(jnp.bfloat16)
            picked = picked + jnp.dot(
                chosen, block_refs[d // per_chunk][d % per_chunk], preferred_element_type=jnp.float32
            )
        total = total + gates[:, k : k + 1] * picked
    out_ref[...] = total.astype(jnp.bfloat16)


def per_device(tokens, routing, gates, norm_gain, w_gate, w_up, w_down):
    tok_count, width = tokens.shape
    top_count = routing.shape[1]
    units = w_gate.shape[2]
    devices = lax.axis_size("ep")
    experts = devices // GROUP
    capacity = GROUP * (5 * tok_count * top_count // (4 * devices))
    chunks = min(MAX_CHUNKS, experts)
    per_chunk = experts // chunks
    place = (lax.axis_index("ep") // GROUP).astype(jnp.int32).reshape(1)

    def swap(x, bit):
        return lax.ppermute(x, "ep", [(i, i ^ bit) for i in range(devices)])

    def travel(x, distance):
        if distance == 0:
            return x
        return lax.ppermute(x, "ep", [(i, (i + GROUP * distance) % devices) for i in range(devices)])

    def along(chunk, c, sign):
        pieces = [travel(chunk[j : j + 1], sign * (c * per_chunk + j)) for j in range(per_chunk)]
        return pieces[0] if per_chunk == 1 else jnp.concatenate(pieces)

    block = jax.ShapeDtypeStruct((per_chunk, capacity, width), jnp.bfloat16)
    in_vmem, in_smem = pl.BlockSpec(memory_space=VMEM), pl.BlockSpec(memory_space=SMEM)
    in_hbm = pl.BlockSpec(memory_space=pl.ANY)
    slots, *blocks = pl.pallas_call(
        functools.partial(prepare_body, experts, capacity),
        out_shape=[jax.ShapeDtypeStruct((tok_count, top_count), jnp.int32)] + [block] * chunks,
        in_specs=[in_smem] + [in_vmem] * 3,
        out_specs=[in_vmem] * (chunks + 1),
        name="prepare",
    )(place, tokens, routing, norm_gain.reshape(1, width))
    others = [swap(w, 1) for w in (w_gate, w_up, w_down)]
    weights = [w for pair in zip((w_gate, w_up, w_down), others) for w in pair]
    half = per_chunk * capacity
    flops = 2 * 2 * half * width * 2 * units * 3
    run = pl.pallas_call(
        expert_body,
        out_shape=[block, block],
        in_specs=[in_vmem] * 2 + [in_hbm] * 6,
        out_specs=[in_vmem] * 2,
        scratch_shapes=[
            VMEM((2 * half, width), jnp.bfloat16),
            VMEM((2 * half, 2 * units), jnp.bfloat16),
            VMEM((2, width, units), jnp.bfloat16),
            VMEM((2, width, units), jnp.bfloat16),
            VMEM((2 * units, width), jnp.bfloat16),
            pltpu.SemaphoreType.DMA((3, 2)),
        ],
        cost_estimate=pl.CostEstimate(
            flops=flops, transcendentals=0, bytes_accessed=2 * 6 * width * units
        ),
        compiler_params=pltpu.CompilerParams(vmem_limit_bytes=40 * 2**20),
        name="expert",
    )
    order = [0, 1, chunks - 1] + list(range(2, chunks - 1)) if chunks > 2 else list(range(chunks))
    arrived = {c: along(blocks[c], c, 1) for c in order}
    crossed = {c: swap(arrived[c], 2) for c in order}
    sums = {c: run(arrived[c], crossed[c], *weights) for c in order}
    back = order[1:] + order[:1]
    finished = {c: (sums[c][0].astype(jnp.float32) + swap(sums[c][1], 2).astype(jnp.float32)).astype(jnp.bfloat16) for c in back}
    returned = [along(finished[c], c, -1) for c in range(chunks)]
    return pl.pallas_call(
        functools.partial(mix_body, experts),
        out_shape=jax.ShapeDtypeStruct((tok_count, width), jnp.bfloat16),
        in_specs=[in_smem] + [in_vmem] * (3 + chunks),
        out_specs=in_vmem,
        name="mix",
    )(place, routing, slots, gates, *returned)


def solution(mesh):
    placed = (
        P(("grp", "ep"), None),
        P(("grp", "ep"), None),
        P(("grp", "ep"), None),
        P(),
        P("ep", None, None),
        P("ep", None, None),
        P("ep", None, None),
    )
    return jax.shard_map(
        per_device, mesh=mesh, in_specs=placed, out_specs=P(("grp", "ep"), None), check_vma=False
    )
```
